256 devices in a mesh: ep: 64 (over z, x, core), tp: 4 (over y).
Axes of the slice: x: 4, y: 4, z: 8, core: 2. Of those that a mesh axis runs over, the one named last changes fastest.
Arguments:
- tokens: bfloat16 [32768, 4096], P('ep', 'tp'), may hold values from -100 to 100, as said below
- routes: int32 [32768, 2], P('ep'), may hold values from 0 to 127, all different within a row; in each aligned block of 512 rows (0 to 511, 512 to 1023, ...) at most 16 rows name the same one
- route_weights: float32 [32768, 2], P('ep'), may hold values from 0.1 to 1
- norm_gain: float32 [4096], P('tp'), may hold values from 0.1 to 1.9
- gate_weight: bfloat16 [128, 4096, 512], P('ep', 'tp'), may hold values from -0.09375 to 0.09375
- up_weight: bfloat16 [128, 4096, 512], P('ep', 'tp'), may hold values from -0.09375 to 0.09375
- down_weight: bfloat16 [128, 512, 4096], P('ep', None, 'tp'), may hold values from -0.25 to 0.25
- final_gain: float32 [4096], P('tp'), may hold values from 0.1 to 1.9
Outputs:
- mixed: bfloat16 [32768, 4096], P('ep', 'tp')
The draws below stay inside these ranges and needn't reach their ends.
Inputs may be any that keep to these rules, and one draw needn't show every extreme that they name: `tokens`: real-valued activations whose features differ in scale. `routes`: each row names 2 different experts; among the 512 rows of one aligned block no expert is named more than 16 times, a bound that some block reaches.
All inputs are finite; a program needn't handle non-finite values.
Results may differ from the reference program's by a relative error of at most 0.018.
Values may be sent and summed in bfloat16 or wider, within the bound.
No kernel may reach another device: no remote copies, remote signals or barrier semaphores. Data moves between devices by JAX's collectives and lax.ppermute only.
A program may use at most 64 MiB of HBM per device.

```python
import math
import jax
import jax.numpy as jnp
import numpy as np
from jax import lax

D = 4096
FF = 512
TOP = 2
TOK_DEV = 512
EXPERTS = 128
CAP = 16
TOKENS = 32768
N_EP = 64
N_TP = 4


def draw_tokens(key, part):
    keys = jax.random.split(jax.random.fold_in(key, 11), 2)
    column = jnp.exp(jnp.log(6.0) * jnp.arange(D, dtype=jnp.float32) / (D - 1))
    row_scale = jnp.exp(jax.random.uniform(keys[1], (TOKENS, 1), jnp.float32, 0.0, jnp.log(10.0)))
    base = jax.random.normal(keys[0], (TOKENS, D), jnp.float32)
    base = jnp.clip(base, -5.0, 5.0)
    return (base * column * row_scale / 3.0).astype(jnp.bfloat16)


def shard_levels(own_key, dims, shards, smallest, high):
    loudness = 1.0
    for dim, blocks in shards:
        draws = jax.random.uniform(jax.random.fold_in(jax.random.fold_in(own_key, 6), dim), (blocks,), jnp.float32, smallest / len(shards), high / len(shards))
        loudness = loudness * jnp.repeat(jnp.exp(draws), dims[dim] // blocks).reshape((-1,) + (1,) * (len(dims) - 1 - dim))
    return loudness


def assign_block(key, own, number, rows, amount, top, limit, skew):
    order = jax.random.permutation(key, amount)
    crowded, ordinary = shares(amount, rows * top, limit, skew, True), shares(amount, rows * top, limit, skew, False)
    places = jnp.arange(amount)

    def named(tallies, offset_by):
        used = int((tallies > 0).sum())
        fixed = max(1, used // 4)
        shifted = fixed + (places - fixed + offset_by * (used - fixed)) % max(1, amount - fixed)
        return jnp.zeros((amount,), jnp.int32).at[order[jnp.where(places < fixed, places, shifted)]].set(jnp.asarray(tallies, jnp.int32))

    tallies = jnp.where(number % 4 == 0, named(crowded, number // 4), named(ordinary, number - number // 4 - 1))
    mixed = jax.random.permutation(jax.random.fold_in(own, 3), amount)
    source_of, sink = mixed[0:amount // 2 * 2:2], mixed[1:amount // 2 * 2:2]
    room = jnp.minimum(tallies[source_of] - 1, limit - tallies[sink]) // 2
    room = jnp.where((source_of == order[0]) | (sink == order[0]) | (tallies[sink] == 0), 0, jnp.maximum(room, 0))
    shifted = jax.random.randint(jax.random.fold_in(own, 4), (amount // 2,), 0, 1 << 20) % (room + 1)
    tallies = tallies.at[source_of].add(-shifted).at[sink].add(shifted)
    labels = jnp.searchsorted(jnp.cumsum(tallies), jnp.arange(rows * top), side="right").astype(jnp.int32)
    listing = labels.reshape(top, rows).T
    listing = listing[jax.random.permutation(jax.random.fold_in(own, 1), rows)]
    offset_by = jax.random.randint(jax.random.fold_in(own, 2), (rows, 1), 0, top)
    return jnp.take_along_axis(listing, (jnp.arange(top)[None, :] + offset_by) % top, axis=1)


def shares(amount, total, reach, lean, full):
    loads = [(1 << 20) // math.isqrt(grade ** lean) + 1 for grade in range(1, amount + 1)]
    largest = reach if full else min(reach, max(-(-total // amount), total * loads[0] // sum(loads)))
    least = 1 if total - largest >= amount - 1 else 0
    given, surplus = [largest] + [least] * (amount - 1), total - largest - least * (amount - 1)
    while surplus > 0:
        candidates = [i for i in range(1, amount) if given[i] < largest] or [i for i in range(1, amount) if given[i] < reach]
        pool, left = sum([loads[i] for i in candidates]), surplus
        for i in candidates:
            addition = min(reach - given[i], max(1, left * loads[i] // pool), surplus)
            given[i] = given[i] + addition
            surplus = surplus - addition
    return np.array(given)


def noise(key, shape, scale, bound, pieces=(), kind=jnp.bfloat16):
    result = scale * jax.random.normal(key, shape, jnp.float32)
    if pieces:
        result = result * shard_levels(key, shape, pieces, -0.22, 0.18)
    return jnp.clip(result, -bound, bound).astype(kind)


def setup_inputs(seed: int = 0) -> dict:
    arg_keys = jax.random.split(jax.random.key(seed), 9)
    tokens = draw_tokens(jax.random.fold_in(arg_keys[8], 71), 0)
    routes_keys = jax.random.split(jax.random.fold_in(arg_keys[1], 1), TOKENS // TOK_DEV)
    routes_turns = jax.random.permutation(jax.random.fold_in(arg_keys[1], 3), TOKENS // TOK_DEV)
    routes = jax.vmap(lambda own, number: assign_block(jax.random.fold_in(arg_keys[1], 2), own, number, TOK_DEV, EXPERTS, TOP, CAP, 2))(routes_keys, routes_turns).reshape((TOKENS, TOP))
    route_weights = jnp.clip(0.1 + 0.9 * jax.random.uniform(arg_keys[2], (TOKENS, TOP), jnp.float32) ** shard_levels(arg_keys[2], (TOKENS, TOP), ((0, 64),), -0.2, 0.2), 0.1, 1.0)
    norm_gain = jnp.clip(1.0 + 0.18 * jax.random.normal(arg_keys[3], (D,), jnp.float32), 0.1, 1.9)
    gate_weight = noise(arg_keys[4], (EXPERTS, D, FF), D ** -0.5, 0.09375, ((0, 64), (1, 4)))
    up_weight = noise(arg_keys[5], (EXPERTS, D, FF), D ** -0.5, 0.09375, ((0, 64), (1, 4)))
    down_weight = noise(arg_keys[6], (EXPERTS, FF, D), FF ** -0.5, 0.25, ((0, 64), (2, 4)))
    final_gain = jnp.clip(1.0 + 0.18 * jax.random.normal(arg_keys[7], (D,), jnp.float32), 0.1, 1.9)
    return {"tokens": tokens, "routes": routes, "route_weights": route_weights, "norm_gain": norm_gain, "gate_weight": gate_weight, "up_weight": up_weight, "down_weight": down_weight, "final_gain": final_gain}


EPSILON = 1e-06

def slots_of(chosen):
    experts = jnp.arange(EXPERTS, dtype=jnp.int32)
    onehot = (chosen[:, None] == experts[None, :]).astype(jnp.int32)
    before = jnp.cumsum(onehot, axis=0) - onehot
    return lax.optimization_barrier(jnp.sum(before * onehot, axis=1)).astype(jnp.int32)

def reference(tokens, routes, route_weights, norm_gain, gate_weight, up_weight, down_weight, final_gain):
    values = tokens.astype(jnp.float32)
    scale = lax.rsqrt(lax.optimization_barrier(jnp.mean(values * values, axis=-1, keepdims=True)) + EPSILON)
    normed = (values * scale * norm_gain).astype(jnp.bfloat16)
    count = tokens.shape[0]
    blocks = routes.reshape(N_EP, TOK_DEV * TOP)
    slots = jax.vmap(slots_of)(blocks)
    source = jnp.broadcast_to(jnp.arange(N_EP, dtype=jnp.int32)[:, None], blocks.shape)
    owner = source * TOK_DEV + jnp.arange(TOK_DEV * TOP, dtype=jnp.int32)[None, :] // TOP
    table = jnp.full((EXPERTS, N_EP, CAP), count, jnp.int32).at[blocks, source, slots].set(owner)
    padded = jnp.concatenate([normed, jnp.zeros((1, D), jnp.bfloat16)], axis=0)
    block_width = D // N_TP

    def one_expert(operands):
        index, w_gate, w_up, w_down = operands
        rows = padded[index.reshape(-1)]
        gate = jnp.zeros((rows.shape[0], FF), jnp.float32)
        upper = jnp.zeros((rows.shape[0], FF), jnp.float32)
        for quarter in range(N_TP):
            lower_col = quarter * block_width
            part_rows = rows[:, lower_col:lower_col + block_width]
            gate = gate + jnp.dot(part_rows, w_gate[lower_col:lower_col + block_width], preferred_element_type=jnp.float32).astype(jnp.bfloat16).astype(jnp.float32)
            upper = upper + jnp.dot(part_rows, w_up[lower_col:lower_col + block_width], preferred_element_type=jnp.float32).astype(jnp.bfloat16).astype(jnp.float32)
        hidden = (jax.nn.silu(gate) * upper).astype(jnp.bfloat16)
        return jnp.dot(hidden, w_down, preferred_element_type=jnp.float32).astype(jnp.bfloat16)
    outputs = lax.map(one_expert, (table, gate_weight, up_weight, down_weight))
    returned = outputs.reshape(EXPERTS * N_EP * CAP, D)
    position = (blocks * (N_EP * CAP) + source * CAP + slots).reshape(count, TOP)
    combined = jnp.zeros((count, D), jnp.float32)
    for which in range(TOP):
        combined = combined + route_weights[:, which:which + 1] * returned[position[:, which]].astype(jnp.float32)
    closing = lax.rsqrt(lax.optimization_barrier(jnp.mean(combined * combined, axis=-1, keepdims=True)) + EPSILON)
    return (combined * closing * final_gain).astype(jnp.bfloat16)
```

```python
import jax
import jax.numpy as jnp
from jax import lax
from jax.sharding import PartitionSpec as P

D = 4096
EPSILON = 1e-06
CHUNKS = 2
F32 = jnp.float32
BF16 = jnp.bfloat16


def shifted(x, axis, by):
    n = lax.axis_size(axis)
    return lax.ppermute(x, axis, [(i, (i + by) % n) for i in range(n)])


def total_over(x, axis):
    parts = [shifted(x, axis, by) for by in range(1, lax.axis_size(axis))]
    for part in parts:
        x = x + part
    return x


def block(x, at, width, dim):
    return lax.dynamic_slice_in_dim(x, at * width, width, dim)


def reduce_scattered(x, axis):
    n = lax.axis_size(axis)
    me = lax.axis_index(axis)
    width = x.shape[1] // n
    acc = block(x, me, width, 1).astype(F32)
    for by in range(1, n):
        acc = acc + shifted(block(x, (me + by) % n, width, 1), axis, by).astype(F32)
    return acc


def gathered(x, axis):
    return [x] + [shifted(x, axis, by) for by in range(1, lax.axis_size(axis))]


def positions(routes, experts):
    rows = routes.shape[0]
    ids = lax.broadcasted_iota(jnp.int32, (experts, rows), 0)
    named = [ids == routes[:, k][None, :] for k in range(routes.shape[1])]
    either = sum(n.astype(BF16) for n in named)
    earlier = (
        lax.broadcasted_iota(jnp.int32, (rows, rows), 0)
        < lax.broadcasted_iota(jnp.int32, (rows, rows), 1)
    ).astype(BF16)
    before = jnp.dot(either, earlier, preferred_element_type=F32)
    return [jnp.sum(jnp.where(n, before, 0.0), axis=0).astype(jnp.int32) for n in named]


def body(tokens, routes, route_weights, norm_gain, gate_weight, up_weight, down_weight, final_gain):
    ep = lax.axis_size("ep")
    members = gate_weight.shape[0]
    experts = ep * members
    rows, width = tokens.shape
    top = routes.shape[1]
    capacity = 4 * rows // experts
    part = capacity // CHUNKS
    values = tokens.astype(F32)
    squares = total_over(jnp.sum(values * values, axis=-1)[None, :], "tp")[0]
    slots = positions(routes, experts)
    normed = (values * lax.rsqrt(squares / D + EPSILON)[:, None] * norm_gain).astype(BF16)
    chunk_rows = experts * part
    ids = lax.broadcasted_iota(jnp.int32, (chunk_rows, rows), 0)

    def placed(c):
        out = []
        for k in range(top):
            inside = (slots[k] >= c * part) & (slots[k] < (c + 1) * part)
            at = jnp.where(inside, routes[:, k] * part + slots[k] - c * part, chunk_rows)
            out.append(ids == at[None, :])
        return out

    def sent(c):
        pick = sum(p.astype(BF16) for p in placed(c))
        rows_out = jnp.dot(pick, normed, preferred_element_type=F32).astype(BF16)
        return lax.all_to_all(
            rows_out.reshape(ep, members * part, width), "ep", 0, 0, tiled=True
        )

    def served(arrived):
        arrived = arrived.reshape(ep, members, part, width)
        hidden_dim = gate_weight.shape[2]
        tp = lax.axis_size("tp")
        partial = []
        for m in range(members):
            r = arrived[:, m].reshape(ep * part, width)
            g = jnp.dot(r, gate_weight[m], preferred_element_type=F32).astype(BF16)
            u = jnp.dot(r, up_weight[m], preferred_element_type=F32).astype(BF16)
            partial.append(jnp.stack([g, u], axis=0))
        both = jnp.stack(partial, axis=0)
        w = hidden_dim // tp
        me = lax.axis_index("tp")
        acc = block(both, me, w, 3).astype(F32)
        for by in range(1, tp):
            acc = acc + shifted(block(both, (me + by) % tp, w, 3), "tp", by).astype(F32)
        share = (jax.nn.silu(acc[:, 0]) * acc[:, 1]).astype(BF16)
        total = 0.0
        for by, piece in enumerate(gathered(share, "tp")):
            wd = block(down_weight, (me - by) % tp, w, 1)
            total = total + jnp.einsum("mrf,mfd->mrd", piece, wd, preferred_element_type=F32)
        out = total.astype(BF16).reshape(members, ep, part, width)
        return jnp.moveaxis(out, 0, 1).reshape(ep, members * part, width)

    arrived = [sent(c) for c in range(CHUNKS)]
    combined = jnp.zeros((rows, width), F32)
    for c in range(CHUNKS):
        back = lax.all_to_all(served(arrived[c]), "ep", 0, 0, tiled=True)
        back = back.reshape(chunk_rows, width)
        weights = sum(
            jnp.where(p, route_weights[:, k][None, :], 0.0) for k, p in enumerate(placed(c))
        )
        high = weights.astype(BF16)
        low = (weights - high.astype(F32)).astype(BF16)
        for w in (high, low):
            combined = combined + lax.dot_general(
                w, back, (((0,), (0,)), ((), ())), preferred_element_type=F32
            )
    closing = total_over(jnp.sum(combined * combined, axis=-1)[None, :], "tp")[0]
    return (combined * lax.rsqrt(closing / D + EPSILON)[:, None] * final_gain).astype(BF16)


def solution(mesh):
    in_specs = (
        P("ep", "tp"),
        P("ep", None),
        P("ep", None),
        P("tp"),
        P("ep", "tp", None),
        P("ep", "tp", None),
        P("ep", None, "tp"),
        P("tp"),
    )
    return jax.shard_map(
        body, mesh=mesh, in_specs=in_specs, out_specs=P("ep", "tp"), check_vma=False
    )
```

```python
import jax
import jax.numpy as jnp
from jax import lax
from jax.sharding import PartitionSpec as P

D = 4096
EPSILON = 1e-06
CHUNKS = 2
F32 = jnp.float32
BF16 = jnp.bfloat16


def shifted(x, axis, by):
    n = lax.axis_size(axis)
    return lax.ppermute(x, axis, [(i, (i + by) % n) for i in range(n)])


def total_over(x, axis):
    parts = [shifted(x, axis, by) for by in range(1, lax.axis_size(axis))]
    for part in parts:
        x = x + part
    return x


def block(x, at, width, dim):
    return lax.dynamic_slice_in_dim(x, at * width, width, dim)


def gathered(x, axis):
    return [x] + [shifted(x, axis, by) for by in range(1, lax.axis_size(axis))]


def positions(routes, experts):
    rows = routes.shape[0]
    ids = lax.broadcasted_iota(jnp.int32, (experts, rows), 0)
    named = [ids == routes[:, k][None, :] for k in range(routes.shape[1])]
    either = sum(n.astype(BF16) for n in named)
    earlier = (
        lax.broadcasted_iota(jnp.int32, (rows, rows), 0)
        < lax.broadcasted_iota(jnp.int32, (rows, rows), 1)
    ).astype(BF16)
    before = jnp.dot(either, earlier, preferred_element_type=F32)
    return [jnp.sum(jnp.where(n, before, 0.0), axis=0).astype(jnp.int32) for n in named]


def layer(tokens, routes, route_weights, norm_gain, gate_weight, up_weight, down_weight, final_gain):
    ep = lax.axis_size("ep")
    members = gate_weight.shape[0]
    experts = ep * members
    rows, width = tokens.shape
    top = routes.shape[1]
    capacity = 4 * rows // experts
    part = capacity // CHUNKS
    values = tokens.astype(F32)
    squares = total_over(jnp.sum(values * values, axis=-1)[None, :], "tp")[0]
    slots = positions(routes, experts)
    normed = (values * lax.rsqrt(squares / D + EPSILON)[:, None] * norm_gain).astype(BF16)
    chunk_rows = experts * part
    ids = lax.broadcasted_iota(jnp.int32, (chunk_rows, rows), 0)

    lanes = lax.broadcasted_iota(jnp.int32, (rows, chunk_rows), 1)

    def places(c):
        out = []
        for k in range(top):
            inside = (slots[k] >= c * part) & (slots[k] < (c + 1) * part)
            out.append(jnp.where(inside, routes[:, k] * part + slots[k] - c * part, chunk_rows))
        return out

    def sent(c):
        pick = sum((ids == p[None, :]).astype(BF16) for p in places(c))
        rows_out = jnp.dot(pick, normed, preferred_element_type=F32).astype(BF16)
        return lax.all_to_all(
            rows_out.reshape(ep, members * part, width), "ep", 0, 0, tiled=True
        )

    def served(arrived):
        arrived = arrived.reshape(ep, members, part, width)
        outs = [one_expert(m, arrived[:, m].reshape(ep * part, width)) for m in range(members)]
        out = jnp.stack([o.reshape(ep, part, width) for o in outs], axis=1)
        return out.reshape(ep, members * part, width)

    def one_expert(m, r):
        tp = lax.axis_size("tp")
        me = lax.axis_index("tp")
        w = gate_weight.shape[2] // tp
        g = jnp.dot(r, gate_weight[m], preferred_element_type=F32).astype(BF16)
        u = jnp.dot(r, up_weight[m], preferred_element_type=F32).astype(BF16)
        both = jnp.stack([g, u], axis=0)
        acc = block(both, me, w, 2).astype(F32)
        for by in range(1, tp):
            acc = acc + shifted(block(both, (me + by) % tp, w, 2), "tp", by).astype(F32)
        share = (jax.nn.silu(acc[0]) * acc[1]).astype(BF16)
        total = 0.0
        for by, piece in enumerate(gathered(share, "tp")):
            wd = block(down_weight[m], (me - by) % tp, w, 0)
            total = total + jnp.dot(piece, wd, preferred_element_type=F32)
        return total.astype(BF16)

    arrived = [sent(c) for c in range(CHUNKS)]
    combined = jnp.zeros((rows, width), F32)
    returned = []
    result = None
    for c in range(CHUNKS):
        block_rows = arrived[c]
        if result is not None:
            block_rows, result = lax.optimization_barrier((block_rows, result))
            returned.append(lax.all_to_all(result, "ep", 0, 0, tiled=True))
        result = served(block_rows)
    returned.append(lax.all_to_all(result, "ep", 0, 0, tiled=True))
    for c, back in enumerate(returned):
        back = back.reshape(chunk_rows, width)
        mix = sum(
            jnp.where(lanes == p[:, None], route_weights[:, k][:, None], 0.0)
            for k, p in enumerate(places(c))
        ).astype(BF16)
        combined = combined + jnp.dot(mix, back, preferred_element_type=F32)
    closing = total_over(jnp.sum(combined * combined, axis=-1)[None, :], "tp")[0]
    return (combined * lax.rsqrt(closing / D + EPSILON)[:, None] * final_gain).astype(BF16)


def solution(mesh):
    in_specs = (
        P("ep", "tp"),
        P("ep", None),
        P("ep", None),
        P("tp"),
        P("ep", "tp", None),
        P("ep", "tp", None),
        P("ep", None, "tp"),
        P("tp"),
    )
    return jax.shard_map(
        layer, mesh=mesh, in_specs=in_specs, out_specs=P("ep", "tp"), check_vma=False
    )
```

```python
import jax
import jax.numpy as jnp
from jax import lax
from jax.sharding import PartitionSpec as P

D = 4096
EPSILON = 1e-06
CHUNKS = 2
F32 = jnp.float32
BF16 = jnp.bfloat16


PAIRS = (((0, 1), (1, 0), (2, 3), (3, 2)), ((0, 3), (3, 0), (1, 2), (2, 1)))


def swapped(x, side):
    return lax.ppermute(x, "tp", PAIRS[side])


def total_over_tp(x):
    for side in (0, 1):
        x = x + swapped(x, side)
    return x


def block(x, at, width, dim):
    return lax.dynamic_slice_in_dim(x, at * width, width, dim)


def positions(routes, experts):
    rows = routes.shape[0]
    ids = lax.broadcasted_iota(jnp.int32, (experts, rows), 0)
    named = [ids == routes[:, k][None, :] for k in range(routes.shape[1])]
    either = sum(n.astype(BF16) for n in named)
    earlier = (
        lax.broadcasted_iota(jnp.int32, (rows, rows), 0)
        < lax.broadcasted_iota(jnp.int32, (rows, rows), 1)
    ).astype(BF16)
    before = jnp.dot(either, earlier, preferred_element_type=F32)
    return [jnp.sum(jnp.where(n, before, 0.0), axis=0).astype(jnp.int32) for n in named]


def layer(tokens, routes, route_weights, norm_gain, gate_weight, up_weight, down_weight, final_gain):
    ep = lax.axis_size("ep")
    members = gate_weight.shape[0]
    experts = ep * members
    rows, width = tokens.shape
    top = routes.shape[1]
    capacity = 4 * rows // experts
    part = capacity // CHUNKS
    values = tokens.astype(F32)
    squares = total_over_tp(jnp.sum(values * values, axis=-1)[None, :])[0]
    slots = positions(routes, experts)
    normed = (values * lax.rsqrt(squares / D + EPSILON)[:, None] * norm_gain).astype(BF16)
    chunk_rows = experts * part
    ids = lax.broadcasted_iota(jnp.int32, (chunk_rows, rows), 0)

    lanes = lax.broadcasted_iota(jnp.int32, (rows, chunk_rows), 1)

    def places(c):
        out = []
        for k in range(top):
            inside = (slots[k] >= c * part) & (slots[k] < (c + 1) * part)
            out.append(jnp.where(inside, routes[:, k] * part + slots[k] - c * part, chunk_rows))
        return out

    def sent(c):
        pick = sum((ids == p[None, :]).astype(BF16) for p in places(c))
        rows_out = jnp.dot(pick, normed, preferred_element_type=F32).astype(BF16)
        return lax.all_to_all(
            rows_out.reshape(ep, members * part, width), "ep", 0, 0, tiled=True
        )

    def served(arrived):
        arrived = arrived.reshape(ep, members, part, width)
        outs = [one_expert(m, arrived[:, m].reshape(ep * part, width)) for m in range(members)]
        out = jnp.stack([o.reshape(ep, part, width) for o in outs], axis=1)
        return out.reshape(ep, members * part, width)

    def one_expert(m, r):
        me = lax.axis_index("tp")
        w = gate_weight.shape[2] // lax.axis_size("tp")
        first, last = m % 2, 1 - m % 2
        near = (me ^ 1, 3 - me)
        far = me ^ 2
        g = jnp.dot(r, gate_weight[m], preferred_element_type=F32).astype(BF16)
        u = jnp.dot(r, up_weight[m], preferred_element_type=F32).astype(BF16)
        both = jnp.stack([g, u], axis=0)
        away = jnp.stack([block(both, near[first], w, 2), block(both, far, w, 2)])
        came = swapped(away, first)
        passed = block(both, near[last], w, 2).astype(F32) + came[1].astype(F32)
        acc = block(both, me, w, 2).astype(F32) + came[0].astype(F32)
        acc = acc + swapped(passed.astype(BF16), last).astype(F32)
        mine = (jax.nn.silu(acc[0]) * acc[1]).astype(BF16)
        pair = jnp.stack([mine, swapped(mine, last)])
        other = swapped(pair, first)
        total = 0.0
        for piece, at in (
            (pair[0], me),
            (pair[1], near[last]),
            (other[0], near[first]),
            (other[1], far),
        ):
            wd = block(down_weight[m], at, w, 0)
            total = total + jnp.dot(piece, wd, preferred_element_type=F32)
        return total.astype(BF16)

    arrived = []
    for c in range(CHUNKS):
        arrived.append(sent(c))
    combined = jnp.zeros((rows, width), F32)
    returned = []
    result = None
    for c in range(CHUNKS):
        block_rows = arrived[c]
        if result is not None:
            block_rows, result = lax.optimization_barrier((block_rows, result))
            returned.append(lax.all_to_all(result, "ep", 0, 0, tiled=True))
        result = served(block_rows)
    returned.append(lax.all_to_all(result, "ep", 0, 0, tiled=True))
    for c, back in enumerate(returned):
        back = back.reshape(chunk_rows, width)
        mix = sum(
            jnp.where(lanes == p[:, None], route_weights[:, k][:, None], 0.0)
            for k, p in enumerate(places(c))
        ).astype(BF16)
        combined = combined + jnp.dot(mix, back, preferred_element_type=F32)
    closing = total_over_tp(jnp.sum(combined * combined, axis=-1)[None, :])[0]
    return (combined * lax.rsqrt(closing / D + EPSILON)[:, None] * final_gain).astype(BF16)


def solution(mesh):
    in_specs = (
        P("ep", "tp"),
        P("ep", None),
        P("ep", None),
        P("tp"),
        P("ep", "tp", None),
        P("ep", "tp", None),
        P("ep", None, "tp"),
        P("tp"),
    )
    return jax.shard_map(
        layer, mesh=mesh, in_specs=in_specs, out_specs=P("ep", "tp"), check_vma=False
    )
```

```python
import jax
import jax.numpy as jnp
from jax import lax
from jax.experimental import pallas as pl
from jax.experimental.pallas import tpu as pltpu
from jax.sharding import PartitionSpec as P

D = 4096
EPSILON = 1e-06
F32 = jnp.float32
BF16 = jnp.bfloat16
HALVES = 2
PAIRS = (((0, 1), (1, 0), (2, 3), (3, 2)), ((0, 3), (3, 0), (1, 2), (2, 1)))


def swapped(x, side):
    return lax.ppermute(x, "tp", PAIRS[side])


def shifted(x, by):
    n = lax.axis_size("tp")
    return lax.ppermute(x, "tp", [(i, (i + by) % n) for i in range(n)])


def total_over_tp(x):
    others = [shifted(x, by) for by in range(1, lax.axis_size("tp"))]
    for other in others:
        x = x + other
    return x


def positions(routes, experts):
    rows = routes.shape[0]
    ids = lax.broadcasted_iota(jnp.int32, (experts, rows), 0)
    named = [ids == routes[:, k][None, :] for k in range(routes.shape[1])]
    either = sum(n.astype(BF16) for n in named)
    earlier = (
        lax.broadcasted_iota(jnp.int32, (rows, rows), 0)
        < lax.broadcasted_iota(jnp.int32, (rows, rows), 1)
    ).astype(BF16)
    before = jnp.dot(either, earlier, preferred_element_type=F32)
    return [jnp.sum(jnp.where(n, before, 0.0), axis=0).astype(jnp.int32) for n in named]


def project_kernel(me_ref, x_ref, gate_ref, up_ref, sent0_ref, sent1_ref, kept0_ref, kept1_ref):
    me = me_ref[0]
    w = sent0_ref.shape[3]
    part = sent0_ref.shape[2]
    x = x_ref[...]
    near0, near1, far = me ^ 1, 3 - me, me ^ 2
    places = (
        (near0, sent0_ref.at[0], kept1_ref.at[0]),
        (near1, kept0_ref.at[0], sent1_ref.at[0]),
        (far, sent0_ref.at[1], sent1_ref.at[1]),
        (me, kept0_ref.at[1], kept1_ref.at[1]),
    )
    for at, *halves in places:
        cols = pl.ds(pl.multiple_of(at * w, w), w)
        weights = jnp.concatenate([gate_ref[0, :, cols], up_ref[0, :, cols]], axis=1)
        out = jnp.dot(x, weights, preferred_element_type=F32).astype(BF16)
        for h, ref in enumerate(halves):
            rows = out[h * part : (h + 1) * part]
            ref[0] = rows[:, :w]
            ref[1] = rows[:, w:]


def projected(rows_in, m, w_gate, w_up):
    tp = lax.axis_size("tp")
    me = jnp.full((1,), lax.axis_index("tp"), jnp.int32)
    members, width, hidden = w_gate.shape
    part = rows_in.shape[0] // HALVES
    out = jax.ShapeDtypeStruct((2, 2, part, hidden // tp), BF16)
    of_member = pl.BlockSpec((1, width, hidden), lambda i: (m, 0, 0))
    return pl.pallas_call(
        project_kernel,
        grid=(1,),
        out_shape=(out,) * 4,
        in_specs=[
            pl.BlockSpec(memory_space=pltpu.SMEM),
            pl.BlockSpec(rows_in.shape, lambda i: (0, 0)),
            of_member,
            of_member,
        ],
        out_specs=(pl.BlockSpec(out.shape, lambda i: (0, 0, 0, 0)),) * 4,
        compiler_params=pltpu.CompilerParams(vmem_limit_bytes=24 * 1024 * 1024),
        cost_estimate=pl.CostEstimate(
            flops=4 * rows_in.size * hidden,
            bytes_accessed=4 * rows_in.size + 4 * w_gate.size // members,
            transcendentals=0,
        ),
    )(me, rows_in, w_gate, w_up)


def served(rows_in, m, w_gate, w_up, w_down):
    tp = lax.axis_size("tp")
    me = lax.axis_index("tp")
    w = w_gate.shape[2] // tp

    def down(share, at):
        wd = lax.dynamic_slice(w_down, (m, at * w, 0), (1, w, w_down.shape[2]))[0]
        return jnp.dot(share, wd, preferred_element_type=F32)

    sent0, sent1, kept0, kept1 = projected(rows_in, m, w_gate, w_up)
    came = [swapped(sent0, 0), swapped(sent1, 1)]
    acc = []
    for h, kept in enumerate((kept0, kept1)):
        passed = kept[0].astype(F32) + came[h][1].astype(F32)
        own = kept[1].astype(F32) + came[h][0].astype(F32)
        acc.append(own + swapped(passed.astype(BF16), 1 - h).astype(F32))
    acc = jnp.concatenate(acc, axis=1)
    mine = (jax.nn.silu(acc[0]) * acc[1]).astype(BF16)
    total = down(mine, me)
    for by in range(1, tp):
        total = total + down(shifted(mine, by), (me - by) % tp)
    return total.astype(BF16)


def layer(tokens, routes, route_weights, norm_gain, gate_weight, up_weight, down_weight, final_gain):
    ep = lax.axis_size("ep")
    members = gate_weight.shape[0]
    experts = ep * members
    rows, width = tokens.shape
    top = routes.shape[1]
    capacity = 4 * rows // experts
    chunk = ep * capacity
    values = tokens.astype(F32)
    squares = total_over_tp(jnp.sum(values * values, axis=-1)[None, :])[0]
    slots = positions(routes, experts)

    def places(m):
        return [
            jnp.where(
                routes[:, k] % members == m, routes[:, k] // members * capacity + slots[k], chunk
            )
            for k in range(top)
        ]

    down_ids = lax.broadcasted_iota(jnp.int32, (chunk, rows), 0)
    across_ids = lax.broadcasted_iota(jnp.int32, (rows, chunk), 1)
    picks = [
        lax.optimization_barrier(sum((down_ids == p[None, :]).astype(BF16) for p in places(m)))
        for m in range(members)
    ]
    normed = (values * lax.rsqrt(squares / D + EPSILON)[:, None] * norm_gain).astype(BF16)

    arrived = []
    for m in range(members):
        rows_out = jnp.dot(picks[m], normed, preferred_element_type=F32).astype(BF16)
        arrived.append(
            lax.all_to_all(rows_out.reshape(ep, capacity, width), "ep", 0, 0, tiled=True)
        )
    returned = []
    result = None
    for m in range(members):
        rows_in = arrived[m].reshape(chunk, width)
        if result is not None:
            rows_in, result = lax.optimization_barrier((rows_in, result))
            returned.append(lax.all_to_all(result, "ep", 0, 0, tiled=True))
        result = served(rows_in, m, gate_weight, up_weight, down_weight)
        result = result.reshape(ep, capacity, width)
    returned.append(lax.all_to_all(result, "ep", 0, 0, tiled=True))
    combined = jnp.zeros((rows, width), F32)
    for m, back in enumerate(returned):
        mix = sum(
            jnp.where(across_ids == p[:, None], route_weights[:, k][:, None], 0.0)
            for k, p in enumerate(places(m))
        ).astype(BF16)
        mix = lax.optimization_barrier(mix)
        combined = combined + jnp.dot(mix, back.reshape(chunk, width), preferred_element_type=F32)
    closing = total_over_tp(jnp.sum(combined * combined, axis=-1)[None, :])[0]
    return (combined * lax.rsqrt(closing / D + EPSILON)[:, None] * final_gain).astype(BF16)


def solution(mesh):
    in_specs = (
        P("ep", "tp"),
        P("ep", None),
        P("ep", None),
        P("tp"),
        P("ep", "tp", None),
        P("ep", "tp", None),
        P("ep", None, "tp"),
        P("tp"),
    )
    return jax.shard_map(
        layer, mesh=mesh, in_specs=in_specs, out_specs=P("ep", "tp"), check_vma=False
    )
```

```python
import functools

import jax
import jax.numpy as jnp
from jax import lax
from jax.experimental import pallas as pl
from jax.experimental.pallas import tpu as pltpu
from jax.sharding import PartitionSpec as P

D = 4096
EPSILON = 1e-06
F32 = jnp.float32
BF16 = jnp.bfloat16
HALVES = 2
PAIRS = (((0, 1), (1, 0), (2, 3), (3, 2)), ((0, 3), (3, 0), (1, 2), (2, 1)))


def swapped(x, side):
    return lax.ppermute(x, "tp", PAIRS[side])


def shifted(x, by):
    n = lax.axis_size("tp")
    return lax.ppermute(x, "tp", [(i, (i + by) % n) for i in range(n)])


def total_over_tp(x):
    others = [shifted(x, by) for by in range(1, lax.axis_size("tp"))]
    for other in others:
        x = x + other
    return x


def positions(routes, experts):
    rows = routes.shape[0]
    ids = lax.broadcasted_iota(jnp.int32, (experts, rows), 0)
    named = [ids == routes[:, k][None, :] for k in range(routes.shape[1])]
    either = sum(n.astype(BF16) for n in named)
    earlier = (
        lax.broadcasted_iota(jnp.int32, (rows, rows), 0)
        < lax.broadcasted_iota(jnp.int32, (rows, rows), 1)
    ).astype(BF16)
    before = jnp.dot(either, earlier, preferred_element_type=F32)
    return [jnp.sum(jnp.where(n, before, 0.0), axis=0).astype(jnp.int32) for n in named]


def project_kernel(
    m,
    me_ref,
    x_ref,
    gain_ref,
    gate_hbm,
    up_hbm,
    sent0_ref,
    sent1_ref,
    kept0_ref,
    kept1_ref,
    gate_ref,
    up_ref,
    gate_sem,
    up_sem,
):
    gate_copy = pltpu.make_async_copy(gate_hbm.at[m], gate_ref, gate_sem)
    up_copy = pltpu.make_async_copy(up_hbm.at[m], up_ref, up_sem)
    gate_copy.start()
    up_copy.start()
    me = me_ref[0]
    w = sent0_ref.shape[3]
    part = sent0_ref.shape[2]
    x = (x_ref[...].astype(F32) * gain_ref[...]).astype(BF16)
    near0, near1, far = me ^ 1, 3 - me, me ^ 2
    gate_copy.wait()
    up_copy.wait()
    places = (
        (near0, sent0_ref.at[0], kept1_ref.at[0]),
        (near1, kept0_ref.at[0], sent1_ref.at[0]),
        (far, sent0_ref.at[1], sent1_ref.at[1]),
        (me, kept0_ref.at[1], kept1_ref.at[1]),
    )
    for at, *halves in places:
        cols = pl.ds(pl.multiple_of(at * w, w), w)
        weights = jnp.concatenate([gate_ref[:, cols], up_ref[:, cols]], axis=1)
        out = jnp.dot(x, weights, preferred_element_type=F32).astype(BF16)
        for h, ref in enumerate(halves):
            rows = out[h * part : (h + 1) * part]
            ref[0] = rows[:, :w]
            ref[1] = rows[:, w:]


def projected(rows_in, gain, m, w_gate, w_up):
    tp = lax.axis_size("tp")
    me = jnp.full((1,), lax.axis_index("tp"), jnp.int32)
    members, width, hidden = w_gate.shape
    part = rows_in.shape[0] // HALVES
    out = jax.ShapeDtypeStruct((2, 2, part, hidden // tp), BF16)
    in_hbm = pl.BlockSpec(memory_space=pltpu.HBM)
    weight = pltpu.VMEM((width, hidden), BF16)
    return pl.pallas_call(
        functools.partial(project_kernel, m),
        grid=(1,),
        out_shape=(out,) * 4,
        in_specs=[
            pl.BlockSpec(memory_space=pltpu.SMEM),
            pl.BlockSpec(rows_in.shape, lambda i: (0, 0)),
            pl.BlockSpec((1, width), lambda i: (0, 0)),
            in_hbm,
            in_hbm,
        ],
        scratch_shapes=[weight, weight, pltpu.SemaphoreType.DMA, pltpu.SemaphoreType.DMA],
        out_specs=(pl.BlockSpec(out.shape, lambda i: (0, 0, 0, 0)),) * 4,
        compiler_params=pltpu.CompilerParams(vmem_limit_bytes=56 * 1024 * 1024),
        cost_estimate=pl.CostEstimate(
            flops=4 * rows_in.size * hidden,
            bytes_accessed=4 * rows_in.size + 4 * w_gate.size // members,
            transcendentals=0,
        ),
    )(me, rows_in, gain[None, :], w_gate, w_up)


def served(rows_in, gain, m, w_gate, w_up, w_down):
    tp = lax.axis_size("tp")
    me = lax.axis_index("tp")
    w = w_gate.shape[2] // tp

    def down(share, at):
        wd = lax.dynamic_slice(w_down, (m, at * w, 0), (1, w, w_down.shape[2]))[0]
        return jnp.dot(share, wd, preferred_element_type=F32)

    sent0, sent1, kept0, kept1 = projected(rows_in, gain, m, w_gate, w_up)
    came = [swapped(sent0, 0), swapped(sent1, 1)]
    values = rows_in.astype(F32)
    squares = jnp.sum(values * values, axis=-1)[None, :]
    for side in (0, 1):
        squares = squares + swapped(squares, side)
    scale = lax.rsqrt(squares[0] / D + EPSILON)[:, None]
    acc = []
    for h, kept in enumerate((kept0, kept1)):
        passed = kept[0].astype(F32) + came[h][1].astype(F32)
        own = kept[1].astype(F32) + came[h][0].astype(F32)
        acc.append(own + swapped(passed.astype(BF16), 1 - h).astype(F32))
    acc = jnp.concatenate(acc, axis=1)
    mine = (jax.nn.silu(acc[0] * scale) * (acc[1] * scale)).astype(BF16)
    total = down(mine, me)
    for by in range(1, tp):
        total = total + down(shifted(mine, by), (me - by) % tp)
    return total.astype(BF16)


def layer(tokens, routes, route_weights, norm_gain, gate_weight, up_weight, down_weight, final_gain):
    ep = lax.axis_size("ep")
    members = gate_weight.shape[0]
    experts = ep * members
    rows, width = tokens.shape
    top = routes.shape[1]
    capacity = 4 * rows // experts
    chunk = ep * capacity
    slots = positions(routes, experts)

    def places(m):
        return [
            jnp.where(
                routes[:, k] % members == m, routes[:, k] // members * capacity + slots[k], chunk
            )
            for k in range(top)
        ]

    down_ids = lax.broadcasted_iota(jnp.int32, (chunk, rows), 0)
    across_ids = lax.broadcasted_iota(jnp.int32, (rows, chunk), 1)
    picks = [
        lax.optimization_barrier(sum((down_ids == p[None, :]).astype(BF16) for p in places(m)))
        for m in range(members)
    ]

    arrived = []
    for m in range(members):
        rows_out = jnp.dot(picks[m], tokens, preferred_element_type=F32).astype(BF16)
        arrived.append(
            lax.all_to_all(rows_out.reshape(ep, capacity, width), "ep", 0, 0, tiled=True)
        )
    returned = []
    result = None
    for m in range(members):
        rows_in = arrived[m].reshape(chunk, width)
        if result is not None:
            rows_in, result = lax.optimization_barrier((rows_in, result))
            returned.append(lax.all_to_all(result, "ep", 0, 0, tiled=True))
        result = served(rows_in, norm_gain, m, gate_weight, up_weight, down_weight)
        result = result.reshape(ep, capacity, width)
    returned.append(lax.all_to_all(result, "ep", 0, 0, tiled=True))
    combined = jnp.zeros((rows, width), F32)
    for m, back in enumerate(returned):
        mix = sum(
            jnp.where(across_ids == p[:, None], route_weights[:, k][:, None], 0.0)
            for k, p in enumerate(places(m))
        ).astype(BF16)
        mix = lax.optimization_barrier(mix)
        combined = combined + jnp.dot(mix, back.reshape(chunk, width), preferred_element_type=F32)
    closing = total_over_tp(jnp.sum(combined * combined, axis=-1)[None, :])[0]
    return (combined * lax.rsqrt(closing / D + EPSILON)[:, None] * final_gain).astype(BF16)


def solution(mesh):
    in_specs = (
        P("ep", "tp"),
        P("ep", None),
        P("ep", None),
        P("tp"),
        P("ep", "tp", None),
        P("ep", "tp", None),
        P("ep", None, "tp"),
        P("tp"),
    )
    return jax.shard_map(
        layer, mesh=mesh, in_specs=in_specs, out_specs=P("ep", "tp"), check_vma=False
    )
```

```python
import jax
import jax.numpy as jnp
from jax import lax
from jax.experimental import pallas as pl
from jax.experimental.pallas import tpu as pltpu
from jax.sharding import PartitionSpec as P

D = 4096
EPSILON = 1e-06
F32 = jnp.float32
BF16 = jnp.bfloat16
HALVES = 2
PAIRS = (((0, 1), (1, 0), (2, 3), (3, 2)), ((0, 3), (3, 0), (1, 2), (2, 1)))


def swapped(x, side):
    return lax.ppermute(x, "tp", PAIRS[side])


def shifted(x, by):
    n = lax.axis_size("tp")
    return lax.ppermute(x, "tp", [(i, (i + by) % n) for i in range(n)])


def total_over_tp(x):
    others = [shifted(x, by) for by in range(1, lax.axis_size("tp"))]
    for other in others:
        x = x + other
    return x


def positions(routes, experts):
    rows = routes.shape[0]
    ids = lax.broadcasted_iota(jnp.int32, (experts, rows), 0)
    named = [ids == routes[:, k][None, :] for k in range(routes.shape[1])]
    either = sum(n.astype(BF16) for n in named)
    earlier = (
        lax.broadcasted_iota(jnp.int32, (rows, rows), 0)
        < lax.broadcasted_iota(jnp.int32, (rows, rows), 1)
    ).astype(BF16)
    before = jnp.dot(either, earlier, preferred_element_type=F32)
    return [jnp.sum(jnp.where(n, before, 0.0), axis=0).astype(jnp.int32) for n in named]


def project_kernel(
    me_ref, x_ref, gain_ref, gate_ref, up_ref, sent0_ref, sent1_ref, kept0_ref, kept1_ref
):
    me = me_ref[0]
    w = sent0_ref.shape[3]
    part = sent0_ref.shape[2]
    x = (x_ref[...].astype(F32) * gain_ref[...]).astype(BF16)
    near0, near1, far = me ^ 1, 3 - me, me ^ 2
    places = (
        (near0, sent0_ref.at[0], kept1_ref.at[0]),
        (near1, kept0_ref.at[0], sent1_ref.at[0]),
        (far, sent0_ref.at[1], sent1_ref.at[1]),
        (me, kept0_ref.at[1], kept1_ref.at[1]),
    )
    for at, *halves in places:
        cols = pl.ds(pl.multiple_of(at * w, w), w)
        weights = jnp.concatenate([gate_ref[0, :, cols], up_ref[0, :, cols]], axis=1)
        out = jnp.dot(x, weights, preferred_element_type=F32).astype(BF16)
        for h, ref in enumerate(halves):
            rows = out[h * part : (h + 1) * part]
            ref[0] = rows[:, :w]
            ref[1] = rows[:, w:]


def projected(rows_in, gain, m, w_gate, w_up):
    tp = lax.axis_size("tp")
    me = jnp.full((1,), lax.axis_index("tp"), jnp.int32)
    members, width, hidden = w_gate.shape
    part = rows_in.shape[0] // HALVES
    out = jax.ShapeDtypeStruct((2, 2, part, hidden // tp), BF16)
    of_member = pl.BlockSpec((1, width, hidden), lambda i: (m, 0, 0))
    return pl.pallas_call(
        project_kernel,
        grid=(1,),
        out_shape=(out,) * 4,
        in_specs=[
            pl.BlockSpec(memory_space=pltpu.SMEM),
            pl.BlockSpec(rows_in.shape, lambda i: (0, 0)),
            pl.BlockSpec((1, width), lambda i: (0, 0)),
            of_member,
            of_member,
        ],
        out_specs=(pl.BlockSpec(out.shape, lambda i: (0, 0, 0, 0)),) * 4,
        compiler_params=pltpu.CompilerParams(vmem_limit_bytes=24 * 1024 * 1024),
        cost_estimate=pl.CostEstimate(
            flops=4 * rows_in.size * hidden,
            bytes_accessed=4 * rows_in.size + 4 * w_gate.size // members,
            transcendentals=0,
        ),
    )(me, rows_in, gain[None, :], w_gate, w_up)


def served(rows_in, gain, m, w_gate, w_up, w_down):
    tp = lax.axis_size("tp")
    me = lax.axis_index("tp")
    w = w_gate.shape[2] // tp

    def down(share, at):
        wd = lax.dynamic_slice(w_down, (m, at * w, 0), (1, w, w_down.shape[2]))[0]
        return jnp.dot(share, wd, preferred_element_type=F32)

    sent0, sent1, kept0, kept1 = projected(rows_in, gain, m, w_gate, w_up)
    came = [swapped(sent0, 0), swapped(sent1, 1)]
    values = rows_in.astype(F32)
    squares = total_over_tp(jnp.sum(values * values, axis=-1)[None, :])
    scale = lax.rsqrt(squares[0] / D + EPSILON)[:, None]
    acc = []
    for h, kept in enumerate((kept0, kept1)):
        passed = kept[0].astype(F32) + came[h][1].astype(F32)
        own = kept[1].astype(F32) + came[h][0].astype(F32)
        acc.append(own + swapped(passed.astype(BF16), 1 - h).astype(F32))
    acc = jnp.concatenate(acc, axis=1)
    mine = (jax.nn.silu(acc[0] * scale) * (acc[1] * scale)).astype(BF16)
    total = down(mine, me)
    for by in range(1, tp):
        total = total + down(shifted(mine, by), (me - by) % tp)
    return total.astype(BF16)


def layer(tokens, routes, route_weights, norm_gain, gate_weight, up_weight, down_weight, final_gain):
    ep = lax.axis_size("ep")
    members = gate_weight.shape[0]
    experts = ep * members
    rows, width = tokens.shape
    top = routes.shape[1]
    capacity = 4 * rows // experts
    chunk = ep * capacity
    slots = positions(routes, experts)

    def places(m):
        return [
            jnp.where(
                routes[:, k] % members == m, routes[:, k] // members * capacity + slots[k], chunk
            )
            for k in range(top)
        ]

    down_ids = lax.broadcasted_iota(jnp.int32, (chunk, rows), 0)
    across_ids = lax.broadcasted_iota(jnp.int32, (rows, chunk), 1)
    picks = [
        lax.optimization_barrier(sum((down_ids == p[None, :]).astype(BF16) for p in places(m)))
        for m in range(members)
    ]

    arrived = []
    for m in range(members):
        rows_out = jnp.dot(picks[m], tokens, preferred_element_type=F32).astype(BF16)
        arrived.append(
            lax.all_to_all(rows_out.reshape(ep, capacity, width), "ep", 0, 0, tiled=True)
        )
    returned = []
    result = None
    for m in range(members):
        rows_in = arrived[m].reshape(chunk, width)
        if result is not None:
            rows_in, result = lax.optimization_barrier((rows_in, result))
            returned.append(lax.all_to_all(result, "ep", 0, 0, tiled=True))
        result = served(rows_in, norm_gain, m, gate_weight, up_weight, down_weight)
        result = result.reshape(ep, capacity, width)
    returned.append(lax.all_to_all(result, "ep", 0, 0, tiled=True))
    combined = jnp.zeros((rows, width), F32)
    for m, back in enumerate(returned):
        mix = sum(
            jnp.where(across_ids == p[:, None], route_weights[:, k][:, None], 0.0)
            for k, p in enumerate(places(m))
        ).astype(BF16)
        mix = lax.optimization_barrier(mix)
        combined = combined + jnp.dot(mix, back.reshape(chunk, width), preferred_element_type=F32)
    closing = total_over_tp(jnp.sum(combined * combined, axis=-1)[None, :])[0]
    return (combined * lax.rsqrt(closing / D + EPSILON)[:, None] * final_gain).astype(BF16)


def solution(mesh):
    in_specs = (
        P("ep", "tp"),
        P("ep", None),
        P("ep", None),
        P("tp"),
        P("ep", "tp", None),
        P("ep", "tp", None),
        P("ep", None, "tp"),
        P("tp"),
    )
    return jax.shard_map(
        layer, mesh=mesh, in_specs=in_specs, out_specs=P("ep", "tp"), check_vma=False
    )
```

```python
import jax
import jax.numpy as jnp
from jax import lax
from jax.experimental import pallas as pl
from jax.experimental.pallas import tpu as pltpu
from jax.sharding import PartitionSpec as P

D = 4096
EPSILON = 1e-06
F32 = jnp.float32
BF16 = jnp.bfloat16
HALVES = 2
TILES = 4
PAIRS = (((0, 1), (1, 0), (2, 3), (3, 2)), ((0, 3), (3, 0), (1, 2), (2, 1)))


def swapped(x, side):
    return lax.ppermute(x, "tp", PAIRS[side])


def shifted(x, by):
    n = lax.axis_size("tp")
    return lax.ppermute(x, "tp", [(i, (i + by) % n) for i in range(n)])


def total_over_tp(x):
    others = [shifted(x, by) for by in range(1, lax.axis_size("tp"))]
    for other in others:
        x = x + other
    return x


def positions(routes, experts):
    rows = routes.shape[0]
    ids = lax.broadcasted_iota(jnp.int32, (experts, rows), 0)
    named = [ids == routes[:, k][None, :] for k in range(routes.shape[1])]
    either = sum(n.astype(BF16) for n in named)
    earlier = (
        lax.broadcasted_iota(jnp.int32, (rows, rows), 0)
        < lax.broadcasted_iota(jnp.int32, (rows, rows), 1)
    ).astype(BF16)
    before = jnp.dot(either, earlier, preferred_element_type=F32)
    return [jnp.sum(jnp.where(n, before, 0.0), axis=0).astype(jnp.int32) for n in named]


def project_kernel(
    me_ref, x_ref, gain_ref, gate_ref, up_ref, sent0_ref, sent1_ref, kept0_ref, kept1_ref
):
    me = me_ref[0]
    w = sent0_ref.shape[3]
    x = (x_ref[...].astype(F32) * gain_ref[...]).astype(BF16)
    second = pl.program_id(0) >= TILES // HALVES
    near0, near1 = me ^ 1, 3 - me
    first, last = jnp.where(second, near1, near0), jnp.where(second, near0, near1)
    outs = []
    for at in (first, me ^ 2, last, me):
        cols = pl.ds(pl.multiple_of(at * w, w), w)
        weights = jnp.concatenate([gate_ref[0, :, cols], up_ref[0, :, cols]], axis=1)
        outs.append(jnp.dot(x, weights, preferred_element_type=F32).astype(BF16))

    def put(sent_ref, kept_ref):
        for i, out in enumerate(outs):
            ref = (sent_ref, kept_ref)[i // 2]
            ref[i % 2, 0] = out[:, :w]
            ref[i % 2, 1] = out[:, w:]

    @pl.when(jnp.logical_not(second))
    def _():
        put(sent0_ref, kept0_ref)

    @pl.when(second)
    def _():
        put(sent1_ref, kept1_ref)


def projected(rows_in, gain, m, w_gate, w_up):
    tp = lax.axis_size("tp")
    me = jnp.full((1,), lax.axis_index("tp"), jnp.int32)
    members, width, hidden = w_gate.shape
    part = rows_in.shape[0] // HALVES
    out = jax.ShapeDtypeStruct((2, 2, part, hidden // tp), BF16)
    of_member = pl.BlockSpec((1, width, hidden), lambda i: (m, 0, 0))
    tile = rows_in.shape[0] // TILES
    per_half = TILES // HALVES
    shape = (2, 2, tile, hidden // tp)
    of_first = pl.BlockSpec(shape, lambda i: (0, 0, jnp.minimum(i, per_half - 1), 0))
    of_second = pl.BlockSpec(shape, lambda i: (0, 0, jnp.maximum(i - per_half, 0), 0))
    return pl.pallas_call(
        project_kernel,
        grid=(TILES,),
        out_shape=(out,) * 4,
        in_specs=[
            pl.BlockSpec(memory_space=pltpu.SMEM),
            pl.BlockSpec((tile, width), lambda i: (i, 0)),
            pl.BlockSpec((1, width), lambda i: (0, 0)),
            of_member,
            of_member,
        ],
        out_specs=(of_first, of_second, of_first, of_second),
        compiler_params=pltpu.CompilerParams(
            vmem_limit_bytes=56 * 1024 * 1024, dimension_semantics=("arbitrary",)
        ),
        cost_estimate=pl.CostEstimate(
            flops=4 * rows_in.size * hidden,
            bytes_accessed=4 * rows_in.size + 4 * w_gate.size // members,
            transcendentals=0,
        ),
    )(me, rows_in, gain[None, :], w_gate, w_up)


def served(rows_in, gain, m, w_gate, w_up, w_down):
    tp = lax.axis_size("tp")
    me = lax.axis_index("tp")
    w = w_gate.shape[2] // tp

    def down(share, at):
        wd = lax.dynamic_slice(w_down, (m, at * w, 0), (1, w, w_down.shape[2]))[0]
        return jnp.dot(share, wd, preferred_element_type=F32)

    sent0, sent1, kept0, kept1 = projected(rows_in, gain, m, w_gate, w_up)
    came = [swapped(sent0, 0), swapped(sent1, 1)]
    values = rows_in.astype(F32)
    squares = total_over_tp(jnp.sum(values * values, axis=-1)[None, :])
    scale = lax.rsqrt(squares[0] / D + EPSILON)[:, None]
    acc = []
    for h, kept in enumerate((kept0, kept1)):
        passed = kept[0].astype(F32) + came[h][1].astype(F32)
        own = kept[1].astype(F32) + came[h][0].astype(F32)
        acc.append(own + swapped(passed.astype(BF16), 1 - h).astype(F32))
    acc = jnp.concatenate(acc, axis=1)
    mine = (jax.nn.silu(acc[0] * scale) * (acc[1] * scale)).astype(BF16)
    total = down(mine, me)
    for by in range(1, tp):
        total = total + down(shifted(mine, by), (me - by) % tp)
    return total.astype(BF16)


def layer(tokens, routes, route_weights, norm_gain, gate_weight, up_weight, down_weight, final_gain):
    ep = lax.axis_size("ep")
    members = gate_weight.shape[0]
    experts = ep * members
    rows, width = tokens.shape
    top = routes.shape[1]
    capacity = 4 * rows // experts
    chunk = ep * capacity
    slots = positions(routes, experts)

    def places(m):
        return [
            jnp.where(
                routes[:, k] % members == m, routes[:, k] // members * capacity + slots[k], chunk
            )
            for k in range(top)
        ]

    down_ids = lax.broadcasted_iota(jnp.int32, (chunk, rows), 0)
    across_ids = lax.broadcasted_iota(jnp.int32, (rows, chunk), 1)
    picks = [
        lax.optimization_barrier(sum((down_ids == p[None, :]).astype(BF16) for p in places(m)))
        for m in range(members)
    ]

    arrived = []
    for m in range(members):
        rows_out = jnp.dot(picks[m], tokens, preferred_element_type=F32).astype(BF16)
        arrived.append(
            lax.all_to_all(rows_out.reshape(ep, capacity, width), "ep", 0, 0, tiled=True)
        )
    returned = []
    result = None
    for m in range(members):
        rows_in = arrived[m].reshape(chunk, width)
        if result is not None:
            rows_in, result = lax.optimization_barrier((rows_in, result))
            returned.append(lax.all_to_all(result, "ep", 0, 0, tiled=True))
        result = served(rows_in, norm_gain, m, gate_weight, up_weight, down_weight)
        result = result.reshape(ep, capacity, width)
    returned.append(lax.all_to_all(result, "ep", 0, 0, tiled=True))
    combined = jnp.zeros((rows, width), F32)
    for m, back in enumerate(returned):
        mix = sum(
            jnp.where(across_ids == p[:, None], route_weights[:, k][:, None], 0.0)
            for k, p in enumerate(places(m))
        ).astype(BF16)
        mix = lax.optimization_barrier(mix)
        combined = combined + jnp.dot(mix, back.reshape(chunk, width), preferred_element_type=F32)
    closing = total_over_tp(jnp.sum(combined * combined, axis=-1)[None, :])[0]
    return (combined * lax.rsqrt(closing / D + EPSILON)[:, None] * final_gain).astype(BF16)


def solution(mesh):
    in_specs = (
        P("ep", "tp"),
        P("ep", None),
        P("ep", None),
        P("tp"),
        P("ep", "tp", None),
        P("ep", "tp", None),
        P("ep", None, "tp"),
        P("tp"),
    )
    return jax.shard_map(
        layer, mesh=mesh, in_specs=in_specs, out_specs=P("ep", "tp"), check_vma=False
    )
```
